32 devices in a mesh: sp: 8 (over z, x), tp: 4 (over y, core).
Axes of the slice: x: 2, y: 2, z: 4, core: 2. Of those that a mesh axis runs over, the one named last changes fastest.
Arguments:
- queries: bfloat16 [3072, 1024], P('sp', 'tp'), may hold values from -160 to 160
- key_vectors: bfloat16 [3072, 1024], P('sp', 'tp'), may hold values from -7 to 7
- values: bfloat16 [3072, 1024], P('sp', 'tp'), may hold values from -6 to 6
- head_lambda: float32 [8], P('tp'), may hold values from 0.3 to 0.8
- head_gain: float32 [128], replicated, may hold values from 0.1 to 1.9
- w_out: bfloat16 [1024, 2048], P('tp'), may hold values from -0.1875 to 0.1875
- residual: bfloat16 [3072, 2048], P(('sp', 'tp')), may hold values from -6 to 6
- ffn_gain: float32 [2048], replicated, may hold values from 0.1 to 1.9
- route_ids: int32 [3072, 2], P(('sp', 'tp')), may hold values from 0 to 7, all different within a row; in each aligned block of 96 rows (0 to 95, 96 to 191, ...) at most 30 rows name the same one
- route_logits: float32 [3072, 2], P(('sp', 'tp')), may hold values from -8 to 310
- w_gate: bfloat16 [8, 2048, 2048], P('sp', None, 'tp'), may hold values from -0.3125 to 0.3125
- w_up: bfloat16 [8, 2048, 2048], P('sp', None, 'tp'), may hold values from -0.3125 to 0.3125
- w_down: bfloat16 [8, 2048, 2048], P('sp', 'tp'), may hold values from -0.125 to 0.125
Outputs:
- layer_out: bfloat16 [3072, 2048], P(('sp', 'tp'))
The draws below stay inside these ranges and needn't reach their ends.
Inputs may be any that keep to these rules, and one draw needn't show every extreme that they name: `route_ids`: in the rows of one device after the attention (aligned blocks of 96 rows) no expert is named by more than 30 rows, a bound that some block reaches while other experts in the same block get fewer rows; each row names 2 different experts.
All inputs are finite; a program needn't handle non-finite values.
Results may differ from the reference program's by a relative error of at most 0.023.
Values may be sent and summed in bfloat16 or wider, within the bound.
A program may use at most 192 MiB of HBM per device.

```python
import math
import jax
import jax.numpy as jnp
import numpy as np
from jax import lax

D = 2048
HEADS = 8
HEAD_DIM = 64
VALUE_DIM = 128
FF = 2048
TOP_K = 2
SEGMENT = 64
SEQ = 3072
LENGTH = 3072
ROWS_DEV = 96
EXPERTS = 8
CAP = 30
N_SP = 8
N_TP = 4


def paired_rows(key):
    width = HEADS * 2 * HEAD_DIM
    query_key = jax.random.fold_in(key, 11)
    key_key = jax.random.fold_in(key, 12)
    query_draw = jnp.clip(jax.random.normal(query_key, (SEQ, width), jnp.float32) * 1.3, -6.5, 6.5)
    key_draw = jnp.clip(jax.random.normal(key_key, (SEQ, width), jnp.float32) * 1.3, -6.5, 6.5)
    return (query_draw, key_draw)


def draw_queries(key, part):
    return paired_rows(key)[0].astype(jnp.bfloat16)


def draw_key_vectors(key, part):
    return paired_rows(key)[1].astype(jnp.bfloat16)


def draw_route_logits(key, part):
    logit_key = jax.random.fold_in(key, 21)
    logits = jnp.clip(jax.random.normal(logit_key, (SEQ, TOP_K), jnp.float32) * 1.5, -8.0, 8.0)
    return logits.astype(jnp.float32)


def level_of(own_key, shape, split, smallest, high):
    loudness, own = 1.0, jax.random.fold_in(own_key, 6)
    for position, parts in split:
        steps = jnp.exp(jax.random.uniform(jax.random.fold_in(own, position), (parts,), jnp.float32, smallest / len(split), high / len(split)))
        loudness = loudness * jnp.repeat(steps, shape[position] // parts).reshape([-1 if axis == position else 1 for axis in range(len(shape))])
    return loudness


def shared_out(rng, own, number, rows, count, top, limit, slope):
    sequence = jax.random.permutation(rng, count)
    heavy_load, ordinary = portions_of(count, rows * top, limit, slope, True), portions_of(count, rows * top, limit, slope, False)
    places = jnp.arange(count)

    def named(sizes, offset_by):
        used = int((sizes > 0).sum())
        fixed = max(1, used // 4)
        shifted = fixed + (places - fixed + offset_by * (used - fixed)) % max(1, count - fixed)
        return jnp.zeros((count,), jnp.int32).at[sequence[jnp.where(places < fixed, places, shifted)]].set(jnp.asarray(sizes, jnp.int32))

    sizes = jnp.where(number % 4 == 0, named(heavy_load, number // 4), named(ordinary, number - number // 4 - 1))
    mixed = jax.random.permutation(jax.random.fold_in(own, 3), count)
    donor, sink = mixed[0:count // 2 * 2:2], mixed[1:count // 2 * 2:2]
    slack = jnp.minimum(sizes[donor] - 1, limit - sizes[sink]) // 2
    slack = jnp.where((donor == sequence[0]) | (sink == sequence[0]) | (sizes[sink] == 0), 0, jnp.maximum(slack, 0))
    shifted = jax.random.randint(jax.random.fold_in(own, 4), (count // 2,), 0, 1 << 20) % (slack + 1)
    sizes = sizes.at[donor].add(-shifted).at[sink].add(shifted)
    items = jnp.searchsorted(jnp.cumsum(sizes), jnp.arange(rows * top), side="right").astype(jnp.int32)
    grid = items.reshape(top, rows).T
    grid = grid[jax.random.permutation(jax.random.fold_in(own, 1), rows)]
    offset_by = jax.random.randint(jax.random.fold_in(own, 2), (rows, 1), 0, top)
    return jnp.take_along_axis(grid, (jnp.arange(top)[None, :] + offset_by) % top, axis=1)


def portions_of(amount, total, limit, skew, full):
    loads = [(1 << 20) // math.isqrt(rank ** skew) + 1 for rank in range(1, amount + 1)]
    largest = limit if full else min(limit, max(-(-total // amount), total * loads[0] // sum(loads)))
    least = 1 if total - largest >= amount - 1 else 0
    given, surplus = [largest] + [least] * (amount - 1), total - largest - least * (amount - 1)
    while surplus > 0:
        candidates = [i for i in range(1, amount) if given[i] < largest] or [i for i in range(1, amount) if given[i] < limit]
        whole, remaining = sum([loads[i] for i in candidates]), surplus
        for i in candidates:
            more = min(limit - given[i], max(1, remaining * loads[i] // whole), surplus)
            given[i] = given[i] + more
            surplus = surplus - more
    return np.array(given)


def bell_draw(stream_key, shape, spread, limit, split=(), held_as=jnp.bfloat16):
    values = spread * jax.random.normal(stream_key, shape, jnp.float32)
    if split:
        values = values * level_of(stream_key, shape, split, -0.22, 0.18)
    return jnp.clip(values, -limit, limit).astype(held_as)


def setup_inputs(seed: int = 0) -> dict:
    arg_keys = jax.random.split(jax.random.key(seed), 14)
    queries = draw_queries(jax.random.fold_in(arg_keys[13], 71), 0)
    key_vectors = draw_key_vectors(jax.random.fold_in(arg_keys[13], 71), 0)
    values = bell_draw(arg_keys[2], (SEQ, HEADS * VALUE_DIM), 1.0, 6.0, ((0, 8), (1, 4)))
    head_lambda = jnp.clip(0.3 + 0.5 * jax.random.uniform(arg_keys[3], (HEADS,), jnp.float32) ** level_of(arg_keys[3], (HEADS,), ((0, 4),), -0.2, 0.2), 0.3, 0.8)
    head_gain = jnp.clip(1.0 + 0.18 * jax.random.normal(arg_keys[4], (VALUE_DIM,), jnp.float32), 0.1, 1.9)
    w_out = bell_draw(arg_keys[5], (HEADS * VALUE_DIM, D), (HEADS * VALUE_DIM) ** -0.5, 0.1875, ((0, 4),))
    residual = bell_draw(arg_keys[6], (SEQ, D), 1.0, 6.0, ((0, 32),))
    ffn_gain = jnp.clip(1.0 + 0.18 * jax.random.normal(arg_keys[7], (D,), jnp.float32), 0.1, 1.9)
    route_ids_keys = jax.random.split(jax.random.fold_in(arg_keys[8], 1), SEQ // ROWS_DEV)
    route_ids_turns = jax.random.permutation(jax.random.fold_in(arg_keys[8], 3), SEQ // ROWS_DEV)
    route_ids = jax.vmap(lambda own, number: shared_out(jax.random.fold_in(arg_keys[8], 2), own, number, ROWS_DEV, EXPERTS, TOP_K, CAP, 2))(route_ids_keys, route_ids_turns).reshape((SEQ, TOP_K))
    route_logits = draw_route_logits(jax.random.fold_in(arg_keys[13], 71), 0)
    w_gate = bell_draw(arg_keys[10], (EXPERTS, D, FF), (D // 6) ** -0.5, 0.3125, ((0, 8), (2, 4)))
    w_up = bell_draw(arg_keys[11], (EXPERTS, D, FF), (D // 6) ** -0.5, 0.3125, ((0, 8), (2, 4)))
    w_down = bell_draw(arg_keys[12], (EXPERTS, FF, D), FF ** -0.5, 0.125, ((0, 8), (1, 4)))
    return dict(queries=queries, key_vectors=key_vectors, values=values, head_lambda=head_lambda, head_gain=head_gain, w_out=w_out, residual=residual, ffn_gain=ffn_gain, route_ids=route_ids, route_logits=route_logits, w_gate=w_gate, w_up=w_up, w_down=w_down)


EPS = 1e-06
NEG = -1e+30
CLAMP = 7.0
ALPHA = 1.702
OUT_FACTOR = 0.8

def attend(queries, key_vectors, values, head_lambda, head_gain):
    seq_len = queries.shape[0]
    query_all = queries.astype(jnp.float32).reshape(seq_len, HEADS, 2, HEAD_DIM)
    key_all = key_vectors.astype(jnp.float32).reshape(seq_len, HEADS, 2, HEAD_DIM)
    value_all = values.astype(jnp.float32).reshape(seq_len, HEADS, VALUE_DIM)
    block_len = math.gcd(256, seq_len)
    key_pos = jnp.arange(seq_len, dtype=jnp.int32)
    key_seg = key_pos // SEGMENT
    key_seq = key_pos // LENGTH
    score_scale = HEAD_DIM ** (-0.5)

    def one_block(block_index):
        first = (block_index * block_len).astype(jnp.int32)
        query_block = lax.dynamic_slice_in_dim(query_all, first, block_len, 0)
        query_pos = first + jnp.arange(block_len, dtype=jnp.int32)
        query_seg = query_pos // SEGMENT
        query_seq = query_pos // LENGTH
        visible = (key_seg[None, :] <= query_seg[:, None]) & (key_seq[None, :] == query_seq[:, None])
        score = jnp.einsum('qhjd,khjd->jhqk', query_block, key_all) * score_scale
        score = jnp.where(visible, score, NEG)
        top = lax.optimization_barrier(jnp.max(score, axis=-1, keepdims=True))
        expo = jnp.where(visible, jnp.exp(score - top), 0.0)
        total = lax.optimization_barrier(jnp.sum(expo, axis=-1))
        weight = lax.optimization_barrier(expo.astype(jnp.bfloat16)).astype(jnp.float32)
        attended = jnp.einsum('jhqk,khd->jqhd', weight, value_all)
        attended = attended / jnp.transpose(total, (0, 2, 1))[..., None]
        diff = attended[0] - head_lambda[None, :, None] * attended[1]
        scale_rows = lax.rsqrt(lax.optimization_barrier(jnp.mean(diff * diff, axis=-1, keepdims=True)) + EPS)
        normed = diff * scale_rows * head_gain * OUT_FACTOR
        return normed.astype(jnp.bfloat16).reshape(block_len, HEADS * VALUE_DIM)
    blocks = lax.map(one_block, jnp.arange(seq_len // block_len, dtype=jnp.int32))
    return blocks.reshape(seq_len, HEADS * VALUE_DIM)

def reference(queries, key_vectors, values, head_lambda, head_gain, w_out, residual, ffn_gain, route_ids, route_logits, w_gate, w_up, w_down):
    head_rows = attend(queries, key_vectors, values, head_lambda, head_gain)
    projected = jnp.dot(head_rows, w_out, preferred_element_type=jnp.float32)
    mixed = (residual.astype(jnp.float32) + projected).astype(jnp.bfloat16)
    mixed32 = mixed.astype(jnp.float32)
    normed = (mixed32 * lax.rsqrt(lax.optimization_barrier(jnp.mean(mixed32 * mixed32, axis=-1, keepdims=True)) + EPS) * ffn_gain).astype(jnp.bfloat16)
    gates = jax.nn.softmax(route_logits, axis=-1)
    bound = N_SP * N_TP * CAP
    flat_ids = route_ids.reshape(-1)
    flat_gates = gates.reshape(-1)
    group = FF // N_TP

    def per_expert(expert, carried):
        order = jnp.argsort(jnp.where(flat_ids == expert, 0, 1).astype(jnp.int32), stable=True)[:bound]
        chosen = (flat_ids[order] == expert).astype(jnp.float32)
        tokens = order // TOP_K
        rows_in = normed[tokens]
        gate_pre = jnp.dot(rows_in, w_gate[expert], preferred_element_type=jnp.float32)
        up_pre = jnp.dot(rows_in, w_up[expert], preferred_element_type=jnp.float32)
        gate_cut = jnp.minimum(gate_pre, CLAMP)
        up_cut = jnp.clip(up_pre, -CLAMP, CLAMP)
        active = (gate_cut * jax.nn.sigmoid(ALPHA * gate_cut) * (up_cut + 1.0)).astype(jnp.bfloat16)
        down = w_down[expert]
        summed = jnp.zeros((bound, D), jnp.float32)
        for quarter in range(N_TP):
            part = jnp.dot(active[:, quarter * group:(quarter + 1) * group], down[quarter * group:(quarter + 1) * group], preferred_element_type=jnp.float32)
            summed = summed + lax.optimization_barrier(part.astype(jnp.bfloat16)).astype(jnp.float32)
        expert_out = lax.optimization_barrier(summed.astype(jnp.bfloat16)).astype(jnp.float32)
        weighted = expert_out * (flat_gates[order] * chosen)[:, None]
        return carried.at[tokens].add(weighted)
    moe_sum = lax.fori_loop(0, EXPERTS, per_expert, jnp.zeros((queries.shape[0], D), jnp.float32))
    return (mixed32 + moe_sum).astype(jnp.bfloat16)
```

```python
import functools

import jax
import jax.numpy as jnp
from jax import lax
from jax.experimental import pallas as pl
from jax.experimental.pallas import tpu as pltpu
from jax.sharding import PartitionSpec as P

SEGMENT = 64
EPS = 1e-06
NEG = -1e30
CLAMP = 7.0
ALPHA = 1.702
OUT_FACTOR = 0.8

MESH = pl.DeviceIdType.MESH
F32 = jnp.float32
BF16 = jnp.bfloat16
VMEM = pl.BlockSpec(memory_space=pltpu.VMEM)
SMEM = pl.BlockSpec(memory_space=pltpu.SMEM)


def remote(src, dst, send_sem, recv_sem, axis, index):
    return pltpu.make_async_remote_copy(
        src_ref=src,
        dst_ref=dst,
        send_sem=send_sem,
        recv_sem=recv_sem,
        device_id={axis: index},
        device_id_type=MESH,
    )


def greet(axis, index):
    barrier = pltpu.get_barrier_semaphore()
    pl.semaphore_signal(barrier, inc=1, device_id={axis: index}, device_id_type=MESH)


def attend_kernel(
    dims, lam_ref, qt_ref, k_ref, vt_ref, gain_ref, out_ref,
    kbuf, vbuf, acc, top, tot, rows_ref, col_send, pair_send, recv, tp_send, tp_recv,
):
    n_sp, n_tp, heads, width, vwidth, toks = dims
    me = lax.axis_index("sp")
    t = lax.axis_index("tp")
    z, x = me // 2, me % 2
    levels = n_sp // 2
    pair = 2 * z + 1 - x
    barrier = pltpu.get_barrier_semaphore()
    greet("sp", pair)
    for d in range(1, n_tp):
        greet("tp", (t + d) % n_tp)

    @pl.when(z > 0)
    def _():
        greet("sp", jnp.maximum(me - 2, 0))

    @pl.when(z < levels - 1)
    def _():
        greet("sp", jnp.minimum(me + 2, n_sp - 1))

    beside = jnp.minimum(z, 1) + jnp.minimum(levels - 1 - z, 1)
    pl.semaphore_wait(barrier, n_tp + beside)
    below = jnp.minimum(me + 2, n_sp - 1)

    def copies(block, k_src, v_src, sems, axis_target):
        return (
            remote(k_src, kbuf.at[block], sems.at[0, block], recv.at[0, block], "sp", axis_target),
            remote(v_src, vbuf.at[block], sems.at[1, block], recv.at[1, block], "sp", axis_target),
        )

    def start(parts):
        for part in parts:
            part.start()

    @pl.when(z < levels - 1)
    def _():
        start(copies(me, k_ref, vt_ref, col_send, below))

    @pl.when(x == 0)
    def _():
        start(copies(me, k_ref, vt_ref, pair_send, pair))

    def absorb(kb, vb, first):
        if first:
            shape = (toks, toks)
            kseg = lax.broadcasted_iota(jnp.int32, shape, 0) // SEGMENT
            qseg = lax.broadcasted_iota(jnp.int32, shape, 1) // SEGMENT
            visible = kseg <= qseg
        for h in range(heads):
            for j in range(2):
                i = 2 * h + j
                keys = kb[:, i * width:(i + 1) * width]
                qs = qt_ref[i * width:(i + 1) * width, :]
                score = jnp.dot(keys, qs, preferred_element_type=F32)
                if first:
                    score = jnp.where(visible, score, NEG)
                high = jnp.max(score, axis=0, keepdims=True)
                if not first:
                    old = top[i:i + 1, :]
                    high = jnp.maximum(high, old)
                expo = jnp.exp(score - high)
                if first:
                    expo = jnp.where(visible, expo, 0.0)
                total = jnp.sum(expo, axis=0, keepdims=True)
                added = jnp.dot(
                    vb[h * vwidth:(h + 1) * vwidth, :], expo.astype(BF16),
                    preferred_element_type=F32,
                )
                if first:
                    acc[i] = added
                else:
                    factor = jnp.exp(old - high)
                    total = total + tot[i:i + 1, :] * factor
                    acc[i] = acc[i] * factor + added
                top[i:i + 1, :] = high
                tot[i:i + 1, :] = total

    absorb(k_ref, vt_ref, True)

    def arrive(block):
        for part in copies(block, k_ref, vt_ref, col_send, me):
            part.wait_recv()

    @pl.when(x == 1)
    def _():
        arrive(pair)
        absorb(kbuf.at[pair], vbuf.at[pair], False)

    def level(c, carry):
        block = me - 2 * (c + 1)
        arrive(block)

        @pl.when(z < levels - 1)
        def _():
            start(copies(block, kbuf.at[block], vbuf.at[block], col_send, below))

        start(copies(block, kbuf.at[block], vbuf.at[block], pair_send, pair))
        absorb(kbuf.at[block], vbuf.at[block], False)
        other = pair - 2 * (c + 1)
        arrive(other)
        absorb(kbuf.at[other], vbuf.at[other], False)
        return carry

    lax.fori_loop(0, z, level, 0)

    for h in range(heads):
        one = acc[2 * h] / tot[2 * h:2 * h + 1, :]
        two = acc[2 * h + 1] / tot[2 * h + 1:2 * h + 2, :]
        diff = one - lam_ref[h] * two
        scale = lax.rsqrt(jnp.mean(diff * diff, axis=0, keepdims=True) + EPS)
        done = diff * scale * gain_ref[...] * OUT_FACTOR
        rows_ref[:, h * vwidth:(h + 1) * vwidth] = done.T.astype(BF16)

    own = toks // n_tp
    span = heads * vwidth
    column = pl.ds(pl.multiple_of(t * span, span), span)
    sends = []
    for d in range(1, n_tp):
        to = (t + d) % n_tp
        row = pl.ds(pl.multiple_of(to * own, own), own)
        sends.append(
            remote(rows_ref.at[row, :], out_ref.at[:, column], tp_send.at[d], tp_recv.at[d], "tp", to)
        )
    start(sends)
    row = pl.ds(pl.multiple_of(t * own, own), own)
    out_ref[:, column] = rows_ref[row, :]

    @pl.when(z < levels - 1)
    def _():
        for part in copies(me, k_ref, vt_ref, col_send, below):
            part.wait_send()

    @pl.when(x == 0)
    def _():
        for part in copies(me, k_ref, vt_ref, pair_send, pair):
            part.wait_send()

    def drain(c, carry):
        block = me - 2 * (c + 1)

        @pl.when(z < levels - 1)
        def _():
            for part in copies(block, k_ref, vt_ref, col_send, below):
                part.wait_send()

        for part in copies(block, k_ref, vt_ref, pair_send, pair):
            part.wait_send()
        return carry

    lax.fori_loop(0, z, drain, 0)
    for part in sends:
        part.wait()


def greet_all(n_sp, me, t):
    barrier = pltpu.get_barrier_semaphore()

    def hello(d, carry):
        greet("sp", (me + d) % n_sp)
        return carry

    lax.fori_loop(1, n_sp, hello, 0)
    greet("tp", t ^ 1)
    greet("tp", t ^ 2)
    pl.semaphore_wait(barrier, n_sp + 1)


def dispatch_kernel(
    n_sp, pick_ref, rows_ref, buf, out, a_send, a_recv, c_send, c_recv, s_send, s_recv,
):
    me = lax.axis_index("sp")
    t = lax.axis_index("tp")
    sib, cross = t ^ 1, t ^ 2
    greet_all(n_sp, me, t)

    def away(p, d):
        return remote(out.at[p], buf.at[t, me], a_send.at[d], a_recv.at[d], "sp", p)

    def send(d, carry):
        p = (me + d) % n_sp
        out[p] = jnp.dot(pick_ref[p], rows_ref[...], preferred_element_type=F32).astype(BF16)
        away(p, d).start()
        return carry

    lax.fori_loop(1, n_sp, send, 0)
    buf[t, me] = jnp.dot(pick_ref[me], rows_ref[...], preferred_element_type=F32).astype(BF16)

    def over(d):
        s = (me + n_sp - d) % n_sp
        mine = buf.at[t, s]
        theirs = buf.at[cross, s]
        return (
            remote(mine, mine, c_send.at[d], c_recv.at[d], "tp", cross),
            remote(mine, mine, s_send.at[0, d], s_recv.at[0, d], "tp", sib),
            remote(theirs, theirs, s_send.at[1, d], s_recv.at[1, d], "tp", sib),
        )

    first = over(0)
    first[0].start()
    first[1].start()

    def step(d, carry):
        away(me, d).wait_recv()
        now = over(d)
        now[0].start()
        now[1].start()
        before = over(d - 1)
        before[0].wait_recv()
        before[2].start()
        return carry

    lax.fori_loop(1, n_sp, step, 0)
    last = over(n_sp - 1)
    last[0].wait_recv()
    last[2].start()

    def drain(d, carry):
        every = over(d)
        every[0].wait_send()
        every[1].wait()
        every[2].wait()

        @pl.when(d > 0)
        def _():
            away(me, d).wait_send()

        return carry

    lax.fori_loop(0, n_sp, drain, 0)


def combine_kernel(
    n_sp, part, ret, ra, rb, stage, fin, s_send, s_recv, c_send, c_recv, a_send, a_recv,
):
    me = lax.axis_index("sp")
    t = lax.axis_index("tp")
    sib, cross = t ^ 1, t ^ 2
    greet_all(n_sp, me, t)

    def place(d):
        return (me + d) % n_sp

    def side(d, which):
        s = place(d)
        owner = sib if which == 0 else sib ^ 2
        return remote(
            part.at[owner, s], ra.at[which, s], s_send.at[which, d], s_recv.at[which, d], "tp", sib
        )

    def over(d):
        s = place(d)
        return remote(stage.at[s], rb.at[s], c_send.at[d], c_recv.at[d], "tp", cross)

    def back(d):
        s = place(d)
        return remote(fin.at[s], ret.at[me], a_send.at[d], a_recv.at[d], "sp", s)

    def begin(i, carry):
        side((i + 1) % n_sp, 1).start()
        side((i + 1) % n_sp, 0).start()
        return carry

    lax.fori_loop(0, n_sp, begin, 0)

    def middle(i, carry):
        d = (i + 1) % n_sp
        s = place(d)
        side(d, 1).wait_recv()
        stage[s] = (part[cross, s].astype(F32) + ra[1, s].astype(F32)).astype(BF16)
        over(d).start()
        return carry

    lax.fori_loop(0, n_sp, middle, 0)

    def total(d):
        s = place(d)
        side(d, 0).wait_recv()
        over(d).wait_recv()
        return (
            part[t, s].astype(F32) + ra[0, s].astype(F32) + rb[s].astype(F32)
        ).astype(BF16)

    def finish(d, carry):
        fin[place(d)] = total(d)
        back(d).start()
        return carry

    lax.fori_loop(1, n_sp, finish, 0)
    ret[me] = total(0)

    def drain(d, carry):
        side(d, 0).wait_send()
        side(d, 1).wait_send()
        over(d).wait_send()

        @pl.when(d > 0)
        def _():
            back(d).wait()

        return carry

    lax.fori_loop(0, n_sp, drain, 0)


def shards(
    queries, key_vectors, values, head_lambda, head_gain, w_out, residual, ffn_gain,
    route_ids, route_logits, w_gate, w_up, w_down,
):
    toks = queries.shape[0]
    heads = head_lambda.shape[0]
    width = queries.shape[1] // (2 * heads)
    vwidth = values.shape[1] // heads
    n_tp = lax.axis_size("tp")
    n_sp = lax.axis_size("sp")
    model = residual.shape[1]
    own = toks // n_tp
    dma = pltpu.SemaphoreType.DMA

    gates = jax.nn.softmax(route_logits, axis=-1)
    top_count = route_ids.shape[1]
    cap = max(2, 5 * top_count * toks // (4 * n_tp * n_sp))
    slots = -(-cap // 16) * 16
    flat_ids = route_ids.reshape(-1)
    chosen = (flat_ids[:, None] == jnp.arange(n_sp, dtype=jnp.int32)[None, :]).astype(jnp.int32)
    earlier = jnp.cumsum(chosen, axis=0) - chosen
    rank = jnp.sum(earlier * chosen, axis=1)
    slot = (flat_ids * slots + rank).reshape(own, top_count)
    lanes = jnp.arange(n_sp * slots, dtype=jnp.int32)
    hits = [(slot[:, k][:, None] == lanes[None, :]).astype(BF16) for k in range(top_count)]
    pick = sum(hits).T.reshape(n_sp, slots, own)

    whole_weight = lax.all_gather(w_out, "tp", axis=0, tiled=True)

    maps = 2 * heads
    scaled = (queries.astype(F32) * width ** (-0.5)).astype(BF16)
    token_heads = pl.pallas_call(
        functools.partial(attend_kernel, (n_sp, n_tp, heads, width, vwidth, toks)),
        out_shape=jax.ShapeDtypeStruct((own, n_tp * heads * vwidth), BF16),
        in_specs=[SMEM, VMEM, VMEM, VMEM, VMEM],
        out_specs=VMEM,
        scratch_shapes=[
            pltpu.VMEM((n_sp,) + key_vectors.shape, BF16),
            pltpu.VMEM((n_sp,) + values.shape[::-1], BF16),
            pltpu.VMEM((maps, vwidth, toks), F32),
            pltpu.VMEM((maps, toks), F32),
            pltpu.VMEM((maps, toks), F32),
            pltpu.VMEM((toks, heads * vwidth), BF16),
            dma((2, n_sp)), dma((2, n_sp)), dma((2, n_sp)), dma((n_tp,)), dma((n_tp,)),
        ],
        compiler_params=pltpu.CompilerParams(collective_id=0, has_side_effects=True),
        cost_estimate=pl.CostEstimate(flops=2 * 10**10, bytes_accessed=10**7, transcendentals=10**6),
        name="attend",
    )(head_lambda, scaled.T, key_vectors, values.T, head_gain.reshape(vwidth, 1))

    projected = jnp.dot(token_heads, whole_weight, preferred_element_type=F32)
    mixed = (residual.astype(F32) + projected).astype(BF16)
    mixed32 = mixed.astype(F32)
    normed = (
        mixed32 * lax.rsqrt(jnp.mean(mixed32 * mixed32, axis=-1, keepdims=True) + EPS) * ffn_gain
    ).astype(BF16)

    piece = pl.pallas_call(
        functools.partial(dispatch_kernel, n_sp),
        out_shape=jax.ShapeDtypeStruct((n_tp, n_sp, slots, model), BF16),
        in_specs=[VMEM, VMEM],
        out_specs=VMEM,
        scratch_shapes=[
            pltpu.VMEM((n_sp, slots, model), BF16),
            dma((n_sp,)), dma((n_sp,)), dma((n_sp,)), dma((n_sp,)), dma((2, n_sp)), dma((2, n_sp)),
        ],
        compiler_params=pltpu.CompilerParams(collective_id=1, has_side_effects=True),
        name="dispatch",
    )(pick, normed)
    piece = piece.reshape(n_tp * n_sp * slots, model)

    gate_pre = jnp.dot(piece, w_gate[0], preferred_element_type=F32)
    up_pre = jnp.dot(piece, w_up[0], preferred_element_type=F32)
    gate_cut = jnp.minimum(gate_pre, CLAMP)
    up_cut = jnp.clip(up_pre, -CLAMP, CLAMP)
    active = (gate_cut * jax.nn.sigmoid(ALPHA * gate_cut) * (up_cut + 1.0)).astype(BF16)
    part = jnp.dot(active, w_down[0], preferred_element_type=F32).astype(BF16)

    returned = pl.pallas_call(
        functools.partial(combine_kernel, n_sp),
        out_shape=jax.ShapeDtypeStruct((n_sp, slots, model), BF16),
        in_specs=[VMEM],
        out_specs=VMEM,
        scratch_shapes=[
            pltpu.VMEM((2, n_sp, slots, model), BF16),
            pltpu.VMEM((n_sp, slots, model), BF16),
            pltpu.VMEM((n_sp, slots, model), BF16),
            pltpu.VMEM((n_sp, slots, model), BF16),
            dma((2, n_sp)), dma((2, n_sp)), dma((n_sp,)), dma((n_sp,)), dma((n_sp,)), dma((n_sp,)),
        ],
        compiler_params=pltpu.CompilerParams(collective_id=2, has_side_effects=True),
        name="combine",
    )(part.reshape(n_tp, n_sp, slots, model))
    returned = returned.reshape(n_sp * slots, model)
    total = mixed32
    for k in range(top_count):
        total = total + gates[:, k:k + 1] * jnp.dot(hits[k], returned, preferred_element_type=F32)
    return total.astype(BF16)


def solution(mesh):
    in_specs = (
        P("sp", "tp"),
        P("sp", "tp"),
        P("sp", "tp"),
        P("tp"),
        P(),
        P("tp", None),
        P(("sp", "tp"), None),
        P(),
        P(("sp", "tp"), None),
        P(("sp", "tp"), None),
        P("sp", None, "tp"),
        P("sp", None, "tp"),
        P("sp", "tp", None),
    )
    out_specs = P(("sp", "tp"), None)
    return jax.shard_map(shards, mesh=mesh, in_specs=in_specs, out_specs=out_specs, check_vma=False)
```

```python
import functools

import jax
import jax.numpy as jnp
from jax import lax
from jax.experimental import pallas as pl
from jax.experimental.pallas import tpu as pltpu
from jax.sharding import PartitionSpec as P

SEGMENT = 64
EPS = 1e-06
NEG = -1e30
CLAMP = 7.0
ALPHA = 1.702
OUT_FACTOR = 0.8

MESH = pl.DeviceIdType.MESH
F32 = jnp.float32
BF16 = jnp.bfloat16
VMEM = pl.BlockSpec(memory_space=pltpu.VMEM)
SMEM = pl.BlockSpec(memory_space=pltpu.SMEM)


def remote(src, dst, send_sem, recv_sem, axis, index):
    return pltpu.make_async_remote_copy(
        src_ref=src,
        dst_ref=dst,
        send_sem=send_sem,
        recv_sem=recv_sem,
        device_id={axis: index},
        device_id_type=MESH,
    )


def greet(axis, index):
    barrier = pltpu.get_barrier_semaphore()
    pl.semaphore_signal(barrier, inc=1, device_id={axis: index}, device_id_type=MESH)


def attend_kernel(
    dims, lam_ref, qt_ref, k_ref, vt_ref, gain_ref, out_ref,
    kbuf, vbuf, acc, top, tot, rows_ref, col_send, pair_send, recv, tp_send, tp_recv,
):
    n_sp, n_tp, heads, width, vwidth, toks = dims
    me = lax.axis_index("sp")
    t = lax.axis_index("tp")
    z, x = me // 2, me % 2
    levels = n_sp // 2
    pair = 2 * z + 1 - x
    barrier = pltpu.get_barrier_semaphore()
    greet("sp", pair)
    for d in range(1, n_tp):
        greet("tp", (t + d) % n_tp)

    @pl.when(z > 0)
    def _():
        greet("sp", jnp.maximum(me - 2, 0))

    @pl.when(z < levels - 1)
    def _():
        greet("sp", jnp.minimum(me + 2, n_sp - 1))

    beside = jnp.minimum(z, 1) + jnp.minimum(levels - 1 - z, 1)
    pl.semaphore_wait(barrier, n_tp + beside)
    below = jnp.minimum(me + 2, n_sp - 1)

    def copies(block, k_src, v_src, sems, axis_target):
        return (
            remote(k_src, kbuf.at[block], sems.at[0, block], recv.at[0, block], "sp", axis_target),
            remote(v_src, vbuf.at[block], sems.at[1, block], recv.at[1, block], "sp", axis_target),
        )

    def start(parts):
        for part in parts:
            part.start()

    @pl.when(z < levels - 1)
    def _():
        start(copies(me, k_ref, vt_ref, col_send, below))

    @pl.when(x == 0)
    def _():
        start(copies(me, k_ref, vt_ref, pair_send, pair))

    def absorb(kb, vb, first):
        if first:
            shape = (toks, toks)
            kseg = lax.broadcasted_iota(jnp.int32, shape, 0) // SEGMENT
            qseg = lax.broadcasted_iota(jnp.int32, shape, 1) // SEGMENT
            visible = kseg <= qseg
        for h in range(heads):
            for j in range(2):
                i = 2 * h + j
                keys = kb[:, i * width:(i + 1) * width]
                qs = qt_ref[i * width:(i + 1) * width, :]
                score = jnp.dot(keys, qs, preferred_element_type=F32)
                if first:
                    score = jnp.where(visible, score, NEG)
                high = jnp.max(score, axis=0, keepdims=True)
                if not first:
                    old = top[i:i + 1, :]
                    high = jnp.maximum(high, old)
                expo = jnp.exp(score - high)
                if first:
                    expo = jnp.where(visible, expo, 0.0)
                total = jnp.sum(expo, axis=0, keepdims=True)
                added = jnp.dot(
                    vb[h * vwidth:(h + 1) * vwidth, :], expo.astype(BF16),
                    preferred_element_type=F32,
                )
                if first:
                    acc[i] = added
                else:
                    factor = jnp.exp(old - high)
                    total = total + tot[i:i + 1, :] * factor
                    acc[i] = acc[i] * factor + added
                top[i:i + 1, :] = high
                tot[i:i + 1, :] = total

    absorb(k_ref, vt_ref, True)

    def arrive(block):
        for part in copies(block, k_ref, vt_ref, col_send, me):
            part.wait_recv()

    @pl.when(x == 1)
    def _():
        arrive(pair)
        absorb(kbuf.at[pair], vbuf.at[pair], False)

    def level(c, carry):
        block = me - 2 * (c + 1)
        arrive(block)

        @pl.when(z < levels - 1)
        def _():
            start(copies(block, kbuf.at[block], vbuf.at[block], col_send, below))

        start(copies(block, kbuf.at[block], vbuf.at[block], pair_send, pair))
        absorb(kbuf.at[block], vbuf.at[block], False)
        other = pair - 2 * (c + 1)
        arrive(other)
        absorb(kbuf.at[other], vbuf.at[other], False)
        return carry

    lax.fori_loop(0, z, level, 0)

    for h in range(heads):
        one = acc[2 * h] / tot[2 * h:2 * h + 1, :]
        two = acc[2 * h + 1] / tot[2 * h + 1:2 * h + 2, :]
        diff = one - lam_ref[h] * two
        scale = lax.rsqrt(jnp.mean(diff * diff, axis=0, keepdims=True) + EPS)
        done = diff * scale * gain_ref[...] * OUT_FACTOR
        rows_ref[:, h * vwidth:(h + 1) * vwidth] = done.T.astype(BF16)

    own = toks // n_tp
    span = heads * vwidth
    column = pl.ds(pl.multiple_of(t * span, span), span)
    sends = []
    for d in range(1, n_tp):
        to = (t + d) % n_tp
        row = pl.ds(pl.multiple_of(to * own, own), own)
        sends.append(
            remote(rows_ref.at[row, :], out_ref.at[:, column], tp_send.at[d], tp_recv.at[d], "tp", to)
        )
    start(sends)
    row = pl.ds(pl.multiple_of(t * own, own), own)
    out_ref[:, column] = rows_ref[row, :]

    @pl.when(z < levels - 1)
    def _():
        for part in copies(me, k_ref, vt_ref, col_send, below):
            part.wait_send()

    @pl.when(x == 0)
    def _():
        for part in copies(me, k_ref, vt_ref, pair_send, pair):
            part.wait_send()

    def drain(c, carry):
        block = me - 2 * (c + 1)

        @pl.when(z < levels - 1)
        def _():
            for part in copies(block, k_ref, vt_ref, col_send, below):
                part.wait_send()

        for part in copies(block, k_ref, vt_ref, pair_send, pair):
            part.wait_send()
        return carry

    lax.fori_loop(0, z, drain, 0)
    for part in sends:
        part.wait()


def experts_kernel(
    n_sp, n_tp, pick_ref, rows_ref, gate_hbm, up_hbm, down_hbm, ret,
    out, buf, part, ra, rb, wg, wu, wd, w_sem,
    a_send, a_recv, c_send, c_recv, s_send, s_recv,
    p_send, p_recv, o_send, o_recv, b_send, b_recv,
):
    me = lax.axis_index("sp")
    t = lax.axis_index("tp")
    sib, cross = t ^ 1, t ^ 2
    slots, model = out.shape[1:]
    chunks = n_sp // 2
    loads = [
        pltpu.make_async_copy(src.at[0], dst, w_sem.at[i])
        for i, (src, dst) in enumerate(((gate_hbm, wg), (up_hbm, wu), (down_hbm, wd)))
    ]
    for load in loads:
        load.start()

    def hello(d, carry):
        greet("sp", me ^ d)
        return carry

    lax.fori_loop(1, n_sp, hello, 0)
    greet("tp", sib)
    greet("tp", cross)
    pl.semaphore_wait(pltpu.get_barrier_semaphore(), n_sp + 1)

    def chosen(p):
        return jnp.dot(pick_ref[p], rows_ref[...], preferred_element_type=F32).astype(BF16)

    def away(d):
        return remote(out.at[d], buf.at[d, t], a_send.at[d], a_recv.at[d], "sp", me ^ d)

    def across(d):
        mine = buf.at[d, t]
        return remote(mine, mine, c_send.at[d], c_recv.at[d], "tp", cross)

    def beside(d, which):
        block = buf.at[d, t if which == 0 else cross]
        return remote(block, block, s_send.at[which, d], s_recv.at[which, d], "tp", sib)

    def side(d, which):
        owner = sib if which == 0 else sib ^ 2
        return remote(
            part.at[d, owner], ra.at[which, d], p_send.at[which, d], p_recv.at[which, d], "tp", sib
        )

    def over(d):
        return remote(part.at[d, cross], rb.at[d], o_send.at[d], o_recv.at[d], "tp", cross)

    def back(d):
        return remote(part.at[d, t], ret.at[me], b_send.at[d], b_recv.at[d], "sp", me ^ d)

    buf[0, t] = chosen(me)

    def send(d, carry):
        out[d] = chosen(me ^ d)
        away(d).start()
        return carry

    lax.fori_loop(1, n_sp, send, 0)
    for load in loads:
        load.wait()

    def forward(d):
        @pl.when(d > 0)
        def _():
            away(d).wait_recv()

        across(d).start()
        beside(d, 0).start()

    def relay(d):
        across(d).wait_recv()
        beside(d, 1).start()

    def multiply(c):
        for d in (2 * c, 2 * c + 1):
            beside(d, 0).wait_recv()
            beside(d, 1).wait_recv()
        rows = buf[pl.ds(2 * c, 2)].reshape(2 * n_tp * slots, model)
        gate = jnp.minimum(jnp.dot(rows, wg[...], preferred_element_type=F32), CLAMP)
        up = jnp.clip(jnp.dot(rows, wu[...], preferred_element_type=F32), -CLAMP, CLAMP)
        active = (gate * jax.nn.sigmoid(ALPHA * gate) * (up + 1.0)).astype(BF16)
        step = 512 if model % 512 == 0 else model
        for first in range(0, model, step):
            piece = jnp.dot(active, wd[:, first:first + step], preferred_element_type=F32)
            part[pl.ds(2 * c, 2), :, :, first:first + step] = piece.astype(BF16).reshape(
                2, n_tp, slots, step
            )
        for d in (2 * c, 2 * c + 1):
            side(d, 1).start()
        for d in (2 * c, 2 * c + 1):
            side(d, 0).start()

    def middle(d):
        side(d, 1).wait_recv()
        part[d, cross] = (part[d, cross].astype(F32) + ra[1, d].astype(F32)).astype(BF16)
        over(d).start()

    def finish(d):
        side(d, 0).wait_recv()
        over(d).wait_recv()
        done = (
            part[d, t].astype(F32) + ra[0, d].astype(F32) + rb[d].astype(F32)
        ).astype(BF16)

        @pl.when(d > 0)
        def _():
            part[d, t] = done
            back(d).start()

        @pl.when(d == 0)
        def _():
            ret[me] = done

    def both(act, c):
        act(2 * c)
        act(2 * c + 1)

    def advance(i, carry):
        @pl.when(i < chunks)
        def _():
            both(forward, i)

        @pl.when((i >= 1) & (i <= chunks))
        def _():
            both(relay, i - 1)
            multiply(i - 1)

        @pl.when(i >= 2)
        def _():
            both(finish, i - 2)

        @pl.when((i >= 1) & (i <= chunks))
        def _():
            both(middle, i - 1)

        return carry

    lax.fori_loop(0, chunks + 2, advance, 0)

    def drain(d, carry):
        across(d).wait_send()
        beside(d, 0).wait_send()
        beside(d, 1).wait_send()
        side(d, 0).wait_send()
        side(d, 1).wait_send()
        over(d).wait_send()

        @pl.when(d > 0)
        def _():
            away(d).wait_send()
            back(d).wait()

        return carry

    lax.fori_loop(0, n_sp, drain, 0)


def shards(
    queries, key_vectors, values, head_lambda, head_gain, w_out, residual, ffn_gain,
    route_ids, route_logits, w_gate, w_up, w_down,
):
    toks = queries.shape[0]
    heads = head_lambda.shape[0]
    width = queries.shape[1] // (2 * heads)
    vwidth = values.shape[1] // heads
    n_tp = lax.axis_size("tp")
    n_sp = lax.axis_size("sp")
    model = residual.shape[1]
    own = toks // n_tp
    dma = pltpu.SemaphoreType.DMA

    gates = jax.nn.softmax(route_logits, axis=-1)
    top_count = route_ids.shape[1]
    cap = max(2, 5 * top_count * toks // (4 * n_tp * n_sp))
    slots = -(-cap // 16) * 16
    flat_ids = route_ids.reshape(-1)
    chosen = (flat_ids[:, None] == jnp.arange(n_sp, dtype=jnp.int32)[None, :]).astype(jnp.int32)
    earlier = jnp.cumsum(chosen, axis=0) - chosen
    rank = jnp.sum(earlier * chosen, axis=1)
    slot = (flat_ids * slots + rank).reshape(own, top_count)
    lanes = jnp.arange(n_sp * slots, dtype=jnp.int32)
    hits = [(slot[:, k][:, None] == lanes[None, :]).astype(BF16) for k in range(top_count)]
    pick = sum(hits).T.reshape(n_sp, slots, own)

    whole_weight = lax.all_gather(w_out, "tp", axis=0, tiled=True)

    maps = 2 * heads
    scaled = (queries.astype(F32) * width ** (-0.5)).astype(BF16)
    token_heads = pl.pallas_call(
        functools.partial(attend_kernel, (n_sp, n_tp, heads, width, vwidth, toks)),
        out_shape=jax.ShapeDtypeStruct((own, n_tp * heads * vwidth), BF16),
        in_specs=[SMEM, VMEM, VMEM, VMEM, VMEM],
        out_specs=VMEM,
        scratch_shapes=[
            pltpu.VMEM((n_sp,) + key_vectors.shape, BF16),
            pltpu.VMEM((n_sp,) + values.shape[::-1], BF16),
            pltpu.VMEM((maps, vwidth, toks), F32),
            pltpu.VMEM((maps, toks), F32),
            pltpu.VMEM((maps, toks), F32),
            pltpu.VMEM((toks, heads * vwidth), BF16),
            dma((2, n_sp)), dma((2, n_sp)), dma((2, n_sp)), dma((n_tp,)), dma((n_tp,)),
        ],
        compiler_params=pltpu.CompilerParams(collective_id=0, has_side_effects=True),
        cost_estimate=pl.CostEstimate(flops=2 * 10**10, bytes_accessed=10**7, transcendentals=10**6),
        name="attend",
    )(head_lambda, scaled.T, key_vectors, values.T, head_gain.reshape(vwidth, 1))

    projected = jnp.dot(token_heads, whole_weight, preferred_element_type=F32)
    mixed = (residual.astype(F32) + projected).astype(BF16)
    mixed32 = mixed.astype(F32)
    normed = (
        mixed32 * lax.rsqrt(jnp.mean(mixed32 * mixed32, axis=-1, keepdims=True) + EPS) * ffn_gain
    ).astype(BF16)

    block = (n_sp, slots, model)
    ff = w_gate.shape[2]
    hbm = pl.BlockSpec(memory_space=pl.ANY)
    lone, twin = dma((n_sp,)), dma((2, n_sp))
    returned = pl.pallas_call(
        functools.partial(experts_kernel, n_sp, n_tp),
        out_shape=jax.ShapeDtypeStruct(block, BF16),
        in_specs=[VMEM, VMEM, hbm, hbm, hbm],
        out_specs=VMEM,
        scratch_shapes=[
            pltpu.VMEM(block, BF16),
            pltpu.VMEM((n_sp, n_tp, slots, model), BF16),
            pltpu.VMEM((n_sp, n_tp, slots, model), BF16),
            pltpu.VMEM((2,) + block, BF16),
            pltpu.VMEM(block, BF16),
            pltpu.VMEM((model, ff), BF16),
            pltpu.VMEM((model, ff), BF16),
            pltpu.VMEM((ff, model), BF16),
            dma((3,)),
            lone, lone, lone, lone, twin, twin, twin, twin, lone, lone, lone, lone,
        ],
        compiler_params=pltpu.CompilerParams(
            collective_id=1, has_side_effects=True, vmem_limit_bytes=67043328
        ),
        name="experts",
    )(pick, normed, w_gate, w_up, w_down)
    returned = returned.reshape(n_sp * slots, model)
    total = mixed32
    for k in range(top_count):
        total = total + gates[:, k:k + 1] * jnp.dot(hits[k], returned, preferred_element_type=F32)
    return total.astype(BF16)


def solution(mesh):
    in_specs = (
        P("sp", "tp"),
        P("sp", "tp"),
        P("sp", "tp"),
        P("tp"),
        P(),
        P("tp", None),
        P(("sp", "tp"), None),
        P(),
        P(("sp", "tp"), None),
        P(("sp", "tp"), None),
        P("sp", None, "tp"),
        P("sp", None, "tp"),
        P("sp", "tp", None),
    )
    out_specs = P(("sp", "tp"), None)
    return jax.shard_map(shards, mesh=mesh, in_specs=in_specs, out_specs=out_specs, check_vma=False)
```
